32 devices in a mesh: fs: 8 (over z, x), tp: 4 (over y, core).
Axes of the slice: x: 2, y: 2, z: 4, core: 2. Of those that a mesh axis runs over, the one named last changes fastest.
Arguments:
- tokens: bfloat16 [3072, 4096], P('fs', 'tp'), may hold values from -600 to 600
- gate_master: float32 [8, 4096, 512], P(None, 'fs', 'tp'), may hold values from -0.09375 to 0.09375
- up_master: float32 [8, 4096, 512], P(None, 'fs', 'tp'), may hold values from -0.09375 to 0.09375
- down_master: float32 [8, 4096, 512], P(None, 'fs', 'tp'), may hold values from -0.25 to 0.25
- norm_gain: float32 [4096], P('fs'), may hold values from 0.1 to 1.9
- routes: int32 [3072, 2], P('fs'), may hold values from 0 to 7, all different within a row; in each aligned block of 384 rows (0 to 383, 384 to 767, ...) at most 192 rows name the same one
- route_weight: float32 [3072, 2], P('fs'), may hold values from 0.1 to 1
Outputs:
- gate_out: bfloat16 [8, 4096, 512], P('fs', None, 'tp')
- up_out: bfloat16 [8, 4096, 512], P('fs', None, 'tp')
- down_out: bfloat16 [8, 4096, 512], P('fs', None, 'tp')
- mixed: bfloat16 [3072, 4096], P('fs', 'tp')
The draws below stay inside these ranges and needn't reach their ends.
Inputs may be any that keep to these rules, and one draw needn't show every extreme that they name: `routes`: within the rows of one index of fs no expert is named by more than 192 pairs, a bound that some block reaches; the 2 experts of a row differ.
All inputs are finite; a program needn't handle non-finite values.
Results may differ from the reference program's by a relative error of at most 0.0087.
Values may be sent and summed in bfloat16 or wider, within the bound.
A program may use at most 128 MiB of HBM per device.

```python
import math
import jax
import jax.numpy as jnp
import numpy as np
from jax import lax

D = 4096
FF = 512
TOP = 2
TOK_DEV = 384
EXPERTS = 8
TOKENS = 3072
CAP = 192
N_FS = 8


def draw_tokens(key, part):
    k_base, k_rows, k_cols = jax.random.split(key, 3)
    row_scale = jnp.exp(jax.random.uniform(k_rows, (TOKENS, 1), jnp.float32) * math.log(10.0))
    position = jnp.arange(D, dtype=jnp.float32)[None, :] / D
    col_scale = jnp.exp(position * math.log(3.0) + jax.random.uniform(k_cols, (1, D), jnp.float32) * math.log(3.3))
    base = jnp.clip(jax.random.normal(k_base, (TOKENS, D), jnp.float32), -6.0, 6.0)
    return (base * row_scale * col_scale).astype(jnp.bfloat16)


def shard_levels(own_key, extent, cuts, low, high):
    def one(dim, shards_of):
        steps = jax.random.uniform(jax.random.fold_in(jax.random.fold_in(own_key, 6), dim), (shards_of,), jnp.float32, low / len(cuts), high / len(cuts))
        return jnp.repeat(jnp.exp(steps), extent[dim] // shards_of).reshape((-1,) + (1,) * (len(extent) - dim - 1))

    factor_of = one(*cuts[0])
    for cut in cuts[1:]:
        factor_of = factor_of * one(*cut)
    return factor_of


def assign_block(own_key, own, number, rows, amount, top, most, slope):
    ranking = jax.random.permutation(own_key, amount)
    packed, ordinary = load_shares(amount, rows * top, most, slope, True), load_shares(amount, rows * top, most, slope, False)
    places = jnp.arange(amount)

    def named(sizes, rotation):
        used = int((sizes > 0).sum())
        fixed = max(1, used // 4)
        passed = fixed + (places - fixed + rotation * (used - fixed)) % max(1, amount - fixed)
        return jnp.zeros((amount,), jnp.int32).at[ranking[jnp.where(places < fixed, places, passed)]].set(jnp.asarray(sizes, jnp.int32))

    sizes = jnp.where(number % 4 == 0, named(packed, number // 4), named(ordinary, number - number // 4 - 1))
    mixed = jax.random.permutation(jax.random.fold_in(own, 3), amount)
    giver, taker = mixed[0:amount // 2 * 2:2], mixed[1:amount // 2 * 2:2]
    room = jnp.minimum(sizes[giver] - 1, most - sizes[taker]) // 2
    room = jnp.where((giver == ranking[0]) | (taker == ranking[0]) | (sizes[taker] == 0), 0, jnp.maximum(room, 0))
    passed = jax.random.randint(jax.random.fold_in(own, 4), (amount // 2,), 0, 1 << 20) % (room + 1)
    sizes = sizes.at[giver].add(-passed).at[taker].add(passed)
    members = jnp.searchsorted(jnp.cumsum(sizes), jnp.arange(rows * top), side="right").astype(jnp.int32)
    grid = members.reshape(top, rows).T
    grid = grid[jax.random.permutation(jax.random.fold_in(own, 1), rows)]
    rotation = jax.random.randint(jax.random.fold_in(own, 2), (rows, 1), 0, top)
    return jnp.take_along_axis(grid, (jnp.arange(top)[None, :] + rotation) % top, axis=1)


def load_shares(number_of, total, reach, skew, full):
    portions = [(1 << 20) // math.isqrt(rank ** skew) + 1 for rank in range(1, number_of + 1)]
    largest = reach if full else min(reach, max(-(-total // number_of), total * portions[0] // sum(portions)))
    least = 1 if total - largest >= number_of - 1 else 0
    holding, surplus = [largest] + [least] * (number_of - 1), total - largest - least * (number_of - 1)
    while surplus > 0:
        free = [i for i in range(1, number_of) if holding[i] < largest] or [i for i in range(1, number_of) if holding[i] < reach]
        pool, remaining = sum([portions[i] for i in free]), surplus
        for i in free:
            addition = min(reach - holding[i], max(1, remaining * portions[i] // pool), surplus)
            holding[i] = holding[i] + addition
            surplus = surplus - addition
    return np.array(holding)


def bell_draw(key, extent, width, bound, shards=(), kind=jnp.bfloat16):
    values = jax.random.normal(key, extent, jnp.float32) * width
    if len(shards) > 0:
        values = shard_levels(key, extent, shards, -0.22, 0.18) * values
    return jnp.clip(values, min=-bound, max=bound).astype(kind)


def setup_inputs(seed: int = 0) -> dict:
    keys = jax.random.split(jax.random.key(seed), 8)
    tokens = draw_tokens(jax.random.fold_in(keys[7], 71), 0)
    gate_master = bell_draw(keys[1], (EXPERTS, D, FF), D ** -0.5, 0.09375, ((1, 8), (2, 4)), jnp.float32)
    up_master = bell_draw(keys[2], (EXPERTS, D, FF), D ** -0.5, 0.09375, ((1, 8), (2, 4)), jnp.float32)
    down_master = bell_draw(keys[3], (EXPERTS, D, FF), FF ** -0.5, 0.25, ((1, 8), (2, 4)), jnp.float32)
    norm_gain = jnp.clip(1.0 + 0.18 * jax.random.normal(keys[4], (D,), jnp.float32), 0.1, 1.9)
    routes_keys = jax.random.split(jax.random.fold_in(keys[5], 1), TOKENS // TOK_DEV)
    routes_turns = jax.random.permutation(jax.random.fold_in(keys[5], 3), TOKENS // TOK_DEV)
    routes = jax.vmap(lambda own, number: assign_block(jax.random.fold_in(keys[5], 2), own, number, TOK_DEV, EXPERTS, TOP, CAP, 2))(routes_keys, routes_turns).reshape((TOKENS, TOP))
    route_weight = jnp.clip(jnp.exp(math.log(1.0) - 2.3025851 * jax.random.uniform(keys[6], (TOKENS, TOP), jnp.float32) ** shard_levels(keys[6], (TOKENS, TOP), ((0, 8),), -0.2, 0.2)), 0.1, 1.0)
    return dict(tokens=tokens, gate_master=gate_master, up_master=up_master, down_master=down_master, norm_gain=norm_gain, routes=routes, route_weight=route_weight)


norm_eps = 1e-06

def slot_table(expert_ids, n_experts, capacity, top_count):
    assigned = expert_ids.shape[0]
    onehot = (expert_ids[:, None] == jnp.arange(n_experts, dtype=jnp.int32)[None, :]).astype(jnp.int32)
    before = jnp.cumsum(onehot, axis=0) - onehot
    slots = lax.optimization_barrier(jnp.sum(before * onehot, axis=1)).astype(jnp.int32)
    position = expert_ids * capacity + slots
    owners = jnp.arange(assigned, dtype=jnp.int32) // top_count
    matches = position[None, :] == jnp.arange(n_experts * capacity, dtype=jnp.int32)[:, None]
    slot_token = lax.optimization_barrier(jnp.max(jnp.where(matches, owners[None, :], -1), axis=1)).astype(jnp.int32)
    return (slots, slot_token)

def reference(tokens, gate_master, up_master, down_master, norm_gain, routes, route_weight):
    folded = norm_gain[None, :, None]
    gate_out = (gate_master * folded).astype(jnp.bfloat16)
    up_out = (up_master * folded).astype(jnp.bfloat16)
    down_out = down_master.astype(jnp.bfloat16)
    token_float = tokens.astype(jnp.float32)
    inverse = lax.rsqrt(lax.optimization_barrier(jnp.mean(token_float * token_float, axis=1, keepdims=True)) + norm_eps)
    normed = (token_float * inverse).astype(jnp.bfloat16)
    mix_weights = route_weight / lax.optimization_barrier(jnp.sum(route_weight, axis=1, keepdims=True))
    block_routes = routes.reshape(N_FS, TOK_DEV * TOP)

    def per_block(one_block):
        return slot_table(one_block, EXPERTS, CAP, TOP)
    slots, slot_token = jax.vmap(per_block)(block_routes)
    offsets = jnp.arange(N_FS, dtype=jnp.int32)[:, None] * TOK_DEV
    global_token = jnp.where(slot_token < 0, TOKENS, slot_token + offsets).astype(jnp.int32)
    padded = jnp.concatenate([normed, jnp.zeros((1, D), jnp.bfloat16)], axis=0)

    def run_expert(expert):
        columns = lax.dynamic_slice_in_dim(global_token, expert * CAP, CAP, 1).reshape(-1)
        expert_rows = padded[columns]
        gate_mat = lax.dynamic_index_in_dim(gate_out, expert, 0, keepdims=False)
        up_mat = lax.dynamic_index_in_dim(up_out, expert, 0, keepdims=False)
        down_mat = lax.dynamic_index_in_dim(down_out, expert, 0, keepdims=False)
        gate_val = jnp.dot(expert_rows, gate_mat, preferred_element_type=jnp.float32)
        up_val = jnp.dot(expert_rows, up_mat, preferred_element_type=jnp.float32)
        hidden = (jax.nn.silu(gate_val) * up_val).astype(jnp.bfloat16)
        result = lax.dot_general(hidden, down_mat, (((1,), (1,)), ((), ())), preferred_element_type=jnp.float32)
        return result.astype(jnp.bfloat16)
    outputs = lax.map(run_expert, jnp.arange(EXPERTS, dtype=jnp.int32))
    flat_out = outputs.reshape(-1, D)
    block_index = jnp.arange(N_FS, dtype=jnp.int32)[:, None]
    index = ((block_routes * N_FS + block_index) * CAP + slots).astype(jnp.int32)
    gathered = flat_out[index.reshape(-1)].astype(jnp.float32).reshape(TOKENS, TOP, D)
    mixed = lax.optimization_barrier(jnp.sum(mix_weights[:, :, None] * gathered, axis=1)).astype(jnp.bfloat16)
    return (gate_out, up_out, down_out, mixed)
```

```python
import jax
import jax.numpy as jnp
from jax import lax
from jax.sharding import PartitionSpec as P

norm_eps = 1e-06


def half_shift(step, size):
    half = size // 2
    return [(s, s // half * half + (s % half + step) % half) for s in range(size)]


def cross_swap(size):
    return [(s, (s + size // 2) % size) for s in range(size)]


def body(tokens, gate_master, up_master, down_master, norm_gain, routes, route_weight):
    n_experts = gate_master.shape[0]
    tok_rows, top_count = routes.shape
    capacity = 2 * tok_rows * top_count // n_experts
    n_tp = lax.axis_size("tp")
    n_fs = lax.axis_size("fs")
    half = n_tp // 2
    width = tokens.shape[1]
    hidden_cols = gate_master.shape[2]
    me_fs = lax.axis_index("fs")
    me_tp = lax.axis_index("tp")

    all_rows = lax.all_gather(tokens, "fs", axis=0)

    folded = norm_gain[None, :, None]
    gate_cast = (gate_master * folded).astype(jnp.bfloat16)
    up_cast = (up_master * folded).astype(jnp.bfloat16)
    down_cast = down_master.astype(jnp.bfloat16)
    gate_out = lax.all_to_all(gate_cast, "fs", split_axis=0, concat_axis=1, tiled=True)
    up_out = lax.all_to_all(up_cast, "fs", split_axis=0, concat_axis=1, tiled=True)
    down_out = lax.all_to_all(down_cast, "fs", split_axis=0, concat_axis=1, tiled=True)

    token_float = tokens.astype(jnp.float32)
    sumsquares = lax.psum(jnp.sum(token_float * token_float, axis=1), "tp")
    inverse = lax.rsqrt(sumsquares / (width * n_tp) + norm_eps)
    mix = route_weight / jnp.sum(route_weight, axis=1, keepdims=True)
    facts = jnp.concatenate([inverse[None], routes.T.astype(jnp.float32), mix.T], axis=0)
    facts = lax.all_gather(facts, "fs", axis=0)
    inverse_all = facts[:, 0]
    named = facts[:, 1 : 1 + top_count] == me_fs.astype(jnp.float32)
    hit = jnp.any(named, axis=1)
    mix_all = jnp.sum(jnp.where(named, facts[:, 1 + top_count :], 0.0), axis=1)
    earlier = jnp.arange(tok_rows)[:, None] < jnp.arange(tok_rows)[None, :]
    slot = jnp.dot(
        hit.astype(jnp.bfloat16), earlier.astype(jnp.bfloat16), preferred_element_type=jnp.float32
    ).astype(jnp.int32)
    place = jnp.where(hit, slot, -1)
    match = place[:, None, :] == jnp.arange(capacity, dtype=jnp.int32)[None, :, None]
    inverse_slot = jnp.sum(jnp.where(match, inverse_all[:, None, :], 0.0), axis=2)
    mix_slot = jnp.sum(jnp.where(match, mix_all[:, None, :], 0.0), axis=2)
    onehot = match.astype(jnp.bfloat16)

    rows = lax.dot_general(
        onehot, all_rows, (((2,), (1,)), ((0,), (0,))), preferred_element_type=jnp.float32
    )
    rows = (rows * inverse_slot[:, :, None]).astype(jnp.bfloat16).reshape(-1, width)

    my_half = me_tp // half
    inside = me_tp % half
    span = half * width
    keep = my_half * span
    give = (1 - my_half) * span

    def rows_of(start):
        return jnp.concatenate(
            [lax.dynamic_slice_in_dim(w[0], start, span, 0) for w in (gate_out, up_out)], axis=1
        )

    own_cols = rows_of(keep)
    partner_cols = lax.ppermute(rows_of(give), "tp", cross_swap(n_tp))

    pieces = [rows] + [lax.ppermute(rows, "tp", half_shift(j, n_tp)) for j in range(1, half)]

    def partial(cols):
        total = 0.0
        for j, piece in enumerate(pieces):
            start = ((inside + half - j) % half) * width
            block = lax.dynamic_slice_in_dim(cols, start, width, 0)
            total = total + jnp.dot(piece, block, preferred_element_type=jnp.float32)
        return total

    for_partner = lax.ppermute(partial(partner_cols).astype(jnp.bfloat16), "tp", cross_swap(n_tp))
    both = partial(own_cols) + for_partner.astype(jnp.float32)
    hidden = (jax.nn.silu(both[:, :hidden_cols]) * both[:, hidden_cols:]).astype(jnp.bfloat16)
    hidden_whole = lax.all_gather(hidden, "tp", axis=1, tiled=True)
    down_quarter = lax.all_to_all(down_out[0], "tp", split_axis=0, concat_axis=1, tiled=True)
    result = lax.dot_general(
        hidden_whole, down_quarter, (((1,), (1,)), ((), ())), preferred_element_type=jnp.float32
    )
    weighted = (result * mix_slot.reshape(-1, 1)).astype(jnp.bfloat16)
    spread = lax.dot_general(
        onehot,
        weighted.reshape(n_fs, capacity, -1),
        (((1,), (1,)), ((0,), (0,))),
        preferred_element_type=jnp.float32,
    ).astype(jnp.bfloat16)
    mixed = lax.psum_scatter(
        spread.reshape(n_fs * tok_rows, -1), "fs", scatter_dimension=0, tiled=True
    )
    return (gate_out, up_out, down_out, mixed)


def solution(mesh):
    placed = (
        P("fs", "tp"),
        P(None, "fs", "tp"),
        P(None, "fs", "tp"),
        P(None, "fs", "tp"),
        P("fs"),
        P("fs", None),
        P("fs", None),
    )
    return jax.shard_map(
        body,
        mesh=mesh,
        in_specs=placed,
        out_specs=(P("fs", None, "tp"), P("fs", None, "tp"), P("fs", None, "tp"), P("fs", "tp")),
        check_vma=False,
    )
```

```python
import jax
import jax.numpy as jnp
from jax import lax
from jax.sharding import PartitionSpec as P

norm_eps = 1e-06


def half_shift(step, size):
    half = size // 2
    return [(s, s // half * half + (s % half + step) % half) for s in range(size)]


def cross_swap(size):
    return [(s, (s + size // 2) % size) for s in range(size)]


def member_shift(step, crossed, size):
    half = size // 2
    return [
        (s, (s // half + crossed) % 2 * half + (s % half + step) % half) for s in range(size)
    ]


def body(tokens, gate_master, up_master, down_master, norm_gain, routes, route_weight):
    n_experts = gate_master.shape[0]
    tok_rows, top_count = routes.shape
    capacity = 2 * tok_rows * top_count // n_experts
    n_tp = lax.axis_size("tp")
    half = n_tp // 2
    width = tokens.shape[1]
    hidden_cols = gate_master.shape[2]
    me_tp = lax.axis_index("tp")
    chunks = 2 if capacity % 32 == 0 else 1
    part = capacity // chunks

    folded = norm_gain[None, :, None]
    pair = jnp.concatenate(
        [(gate_master * folded).astype(jnp.bfloat16), (up_master * folded).astype(jnp.bfloat16)], axis=2
    )
    pair = lax.all_to_all(pair, "fs", split_axis=0, concat_axis=1, tiled=True)
    down_cast, pair = lax.optimization_barrier((down_master.astype(jnp.bfloat16), pair))
    down_out = lax.all_to_all(down_cast, "fs", split_axis=0, concat_axis=1, tiled=True)
    gate_out = pair[:, :, :hidden_cols]
    up_out = pair[:, :, hidden_cols:]

    token_float = tokens.astype(jnp.float32)
    sumsquares = lax.psum(jnp.sum(token_float * token_float, axis=1), "tp")
    inverse = lax.rsqrt(sumsquares / (width * n_tp) + norm_eps)[:, None]
    normed = (token_float * inverse).astype(jnp.bfloat16)
    mix = route_weight / jnp.sum(route_weight, axis=1, keepdims=True)
    experts = jnp.arange(n_experts, dtype=jnp.int32)
    named = jnp.any(routes[:, :, None] == experts, axis=1)
    earlier = jnp.arange(tok_rows)[:, None] > jnp.arange(tok_rows)[None, :]
    before = jnp.dot(
        earlier.astype(jnp.bfloat16), named.astype(jnp.bfloat16), preferred_element_type=jnp.float32
    ).astype(jnp.int32)
    slots = jnp.sum(jnp.where(routes[:, :, None] == experts, before[:, None, :], 0), axis=2)
    place = (slots // part * n_experts + routes) * part + slots % part
    spots = jnp.arange(n_experts * capacity, dtype=jnp.int32)
    where_to = place[:, :, None] == spots
    onehot = jnp.any(where_to, axis=1).astype(jnp.bfloat16)
    mixing = jnp.sum(jnp.where(where_to, mix[:, :, None], 0.0), axis=1)
    mixing_high = mixing.astype(jnp.bfloat16)
    mixing_low = (mixing - mixing_high.astype(jnp.float32)).astype(jnp.bfloat16)
    outgoing = lax.dot_general(
        onehot, normed, (((0,), (0,)), ((), ())), preferred_element_type=jnp.float32
    ).astype(jnp.bfloat16)
    outgoing = outgoing.reshape(chunks, n_experts, part, width)

    my_half = me_tp // half
    inside = me_tp % half
    span = half * width
    own_cols = lax.dynamic_slice_in_dim(pair[0], my_half * span, span, 0)
    partner_cols = lax.ppermute(
        lax.dynamic_slice_in_dim(pair[0], (1 - my_half) * span, span, 0), "tp", cross_swap(n_tp)
    )

    arrived = []
    for c in range(chunks):
        if c == 0:
            ready, down_out, partner_cols = lax.optimization_barrier((outgoing[c], down_out, partner_cols))
        else:
            ready, arrived[-1] = lax.optimization_barrier((outgoing[c], last))
        last = lax.all_to_all(ready, "fs", split_axis=0, concat_axis=0, tiled=True)
        arrived.append(last)

    def in_order(cols):
        blocks = cols.reshape(half, width, cols.shape[1])
        return [
            lax.dynamic_index_in_dim(blocks, (inside + half - j) % half, 0, keepdims=False)
            for j in range(half)
        ]

    own_blocks, partner_blocks = in_order(own_cols), in_order(partner_cols)
    quarters = down_out[0].reshape(n_tp, -1, hidden_cols)
    picked = []
    for j in range(half):
        for crossed in range(2):
            target = (my_half + crossed) % 2 * half + (inside + j) % half
            piece = lax.dynamic_index_in_dim(quarters, target, 0, keepdims=False)
            if j + crossed > 0:
                piece = lax.ppermute(piece, "tp", member_shift(j, crossed, n_tp))
            picked.append(piece)
    down_mat = jnp.concatenate(picked, axis=1)

    def serve(rows):
        rows = rows.reshape(-1, width)
        pieces = [rows] + [lax.ppermute(rows, "tp", half_shift(j, n_tp)) for j in range(1, half)]

        def partial(blocks):
            total = 0.0
            for piece, block in zip(pieces, blocks):
                total = total + jnp.dot(piece, block, preferred_element_type=jnp.float32)
            return total

        swapped = lax.ppermute(partial(partner_blocks).astype(jnp.bfloat16), "tp", cross_swap(n_tp))
        both = partial(own_blocks) + swapped.astype(jnp.float32)
        hidden = (jax.nn.silu(both[:, :hidden_cols]) * both[:, hidden_cols:]).astype(jnp.bfloat16)
        two = jnp.concatenate([hidden, lax.ppermute(hidden, "tp", cross_swap(n_tp))], axis=1)
        all_hidden = [two] + [lax.ppermute(two, "tp", half_shift(j, n_tp)) for j in range(1, half)]
        result = lax.dot_general(
            jnp.concatenate(all_hidden, axis=1),
            down_mat,
            (((1,), (1,)), ((), ())),
            preferred_element_type=jnp.float32,
        )
        return result.astype(jnp.bfloat16).reshape(-1, part, width)

    returned = []
    for c in range(chunks):
        rows = arrived[c]
        if c > 0:
            rows, served = lax.optimization_barrier((rows, served))
            returned.append(lax.all_to_all(served, "fs", split_axis=0, concat_axis=0, tiled=True))
        served = serve(rows)
    returned.append(lax.all_to_all(served, "fs", split_axis=0, concat_axis=0, tiled=True))

    mixed = 0.0
    for c, back in enumerate(returned):
        flat = back.reshape(n_experts * part, width)
        for weights in (mixing_high, mixing_low):
            chosen = weights[:, c * n_experts * part : (c + 1) * n_experts * part]
            mixed = mixed + jnp.dot(chosen, flat, preferred_element_type=jnp.float32)
    return (gate_out, up_out, down_out, mixed.astype(jnp.bfloat16))


def solution(mesh):
    placed = (
        P("fs", "tp"),
        P(None, "fs", "tp"),
        P(None, "fs", "tp"),
        P(None, "fs", "tp"),
        P("fs"),
        P("fs", None),
        P("fs", None),
    )
    return jax.shard_map(
        body,
        mesh=mesh,
        in_specs=placed,
        out_specs=(P("fs", None, "tp"), P("fs", None, "tp"), P("fs", None, "tp"), P("fs", "tp")),
        check_vma=False,
    )
```

```python
import jax
import jax.numpy as jnp
from jax import lax
from jax.sharding import PartitionSpec as P

norm_eps = 1e-06


def half_shift(step, size):
    half = size // 2
    return [(s, s // half * half + (s % half + step) % half) for s in range(size)]


def cross_swap(size):
    return [(s, (s + size // 2) % size) for s in range(size)]


def member_shift(step, crossed, size):
    half = size // 2
    return [
        (s, (s // half + crossed) % 2 * half + (s % half + step) % half) for s in range(size)
    ]


def body(tokens, gate_master, up_master, down_master, norm_gain, routes, route_weight):
    n_experts = gate_master.shape[0]
    tok_rows, top_count = routes.shape
    capacity = 2 * tok_rows * top_count // n_experts
    n_tp = lax.axis_size("tp")
    half = n_tp // 2
    width = tokens.shape[1]
    hidden_cols = gate_master.shape[2]
    me_tp = lax.axis_index("tp")
    chunks = 2 if capacity % 32 == 0 else 1
    part = capacity // chunks

    folded = norm_gain[None, :, None]
    trio = jnp.concatenate(
        [
            (gate_master * folded).astype(jnp.bfloat16),
            (up_master * folded).astype(jnp.bfloat16),
            down_master.astype(jnp.bfloat16),
        ],
        axis=2,
    )
    trio = lax.all_to_all(trio, "fs", split_axis=0, concat_axis=1, tiled=True)
    pair = trio[:, :, : 2 * hidden_cols]
    gate_out = trio[:, :, :hidden_cols]
    up_out = trio[:, :, hidden_cols : 2 * hidden_cols]
    down_out = trio[:, :, 2 * hidden_cols :]

    token_float = tokens.astype(jnp.float32)
    sumsquares = lax.psum(jnp.sum(token_float * token_float, axis=1), "tp")
    inverse = lax.rsqrt(sumsquares / (width * n_tp) + norm_eps)[:, None]
    normed = (token_float * inverse).astype(jnp.bfloat16)
    mix = route_weight / jnp.sum(route_weight, axis=1, keepdims=True)
    experts = jnp.arange(n_experts, dtype=jnp.int32)
    named = jnp.any(routes[:, :, None] == experts, axis=1)
    earlier = jnp.arange(tok_rows)[:, None] > jnp.arange(tok_rows)[None, :]
    before = jnp.dot(
        earlier.astype(jnp.bfloat16), named.astype(jnp.bfloat16), preferred_element_type=jnp.float32
    ).astype(jnp.int32)
    slots = jnp.sum(jnp.where(routes[:, :, None] == experts, before[:, None, :], 0), axis=2)
    place = (slots // part * n_experts + routes) * part + slots % part
    spots = jnp.arange(n_experts * capacity, dtype=jnp.int32)
    where_to = place[:, :, None] == spots
    onehot = jnp.any(where_to, axis=1).astype(jnp.bfloat16)
    mixing = jnp.sum(jnp.where(where_to, mix[:, :, None], 0.0), axis=1)
    mixing = mixing.astype(jnp.bfloat16)
    outgoing = lax.dot_general(
        onehot, normed, (((0,), (0,)), ((), ())), preferred_element_type=jnp.float32
    ).astype(jnp.bfloat16)
    outgoing = outgoing.reshape(chunks, n_experts, part, width)

    my_half = me_tp // half
    inside = me_tp % half
    span = half * width
    own_cols = lax.dynamic_slice_in_dim(pair[0], my_half * span, span, 0)
    partner_cols = lax.ppermute(
        lax.dynamic_slice_in_dim(pair[0], (1 - my_half) * span, span, 0), "tp", cross_swap(n_tp)
    )

    arrived = []
    for c in range(chunks):
        if c == 0:
            ready, trio = lax.optimization_barrier((outgoing[c], trio))
        else:
            ready, arrived[-1], partner_cols = lax.optimization_barrier((outgoing[c], last, partner_cols))
        last = lax.all_to_all(ready, "fs", split_axis=0, concat_axis=0, tiled=True)
        arrived.append(last)

    def in_order(cols):
        blocks = cols.reshape(half, width, cols.shape[1])
        return [
            lax.dynamic_index_in_dim(blocks, (inside + half - j) % half, 0, keepdims=False)
            for j in range(half)
        ]

    own_blocks, partner_blocks = in_order(own_cols), in_order(partner_cols)
    quarters = down_out[0].reshape(n_tp, -1, hidden_cols)
    picked = []
    for j in range(half):
        for crossed in range(2):
            target = (my_half + crossed) % 2 * half + (inside + j) % half
            piece = lax.dynamic_index_in_dim(quarters, target, 0, keepdims=False)
            if j + crossed > 0:
                piece = lax.ppermute(piece, "tp", member_shift(j, crossed, n_tp))
            picked.append(piece)
    down_mat = jnp.concatenate(picked, axis=1)

    def serve(rows):
        rows = rows.reshape(-1, width)
        pieces = [rows] + [lax.ppermute(rows, "tp", half_shift(j, n_tp)) for j in range(1, half)]

        def partial(blocks):
            total = 0.0
            for piece, block in zip(pieces, blocks):
                total = total + jnp.dot(piece, block, preferred_element_type=jnp.float32)
            return total

        swapped = lax.ppermute(partial(partner_blocks).astype(jnp.bfloat16), "tp", cross_swap(n_tp))
        both = partial(own_blocks) + swapped.astype(jnp.float32)
        hidden = (jax.nn.silu(both[:, :hidden_cols]) * both[:, hidden_cols:]).astype(jnp.bfloat16)
        two = jnp.concatenate([hidden, lax.ppermute(hidden, "tp", cross_swap(n_tp))], axis=1)
        all_hidden = [two] + [lax.ppermute(two, "tp", half_shift(j, n_tp)) for j in range(1, half)]
        result = lax.dot_general(
            jnp.concatenate(all_hidden, axis=1),
            down_mat,
            (((1,), (1,)), ((), ())),
            preferred_element_type=jnp.float32,
        )
        return result.astype(jnp.bfloat16).reshape(-1, part, width)

    returned = []
    for c in range(chunks):
        rows = arrived[c]
        if c > 0:
            rows, served = lax.optimization_barrier((rows, served))
            returned.append(lax.all_to_all(served, "fs", split_axis=0, concat_axis=0, tiled=True))
        served = serve(rows)
    returned.append(lax.all_to_all(served, "fs", split_axis=0, concat_axis=0, tiled=True))

    mixed = 0.0
    for c, back in enumerate(returned):
        flat = back.reshape(n_experts * part, width)
        chosen = mixing[:, c * n_experts * part : (c + 1) * n_experts * part]
        mixed = mixed + jnp.dot(chosen, flat, preferred_element_type=jnp.float32)
    return (gate_out, up_out, down_out, mixed.astype(jnp.bfloat16))


def solution(mesh):
    placed = (
        P("fs", "tp"),
        P(None, "fs", "tp"),
        P(None, "fs", "tp"),
        P(None, "fs", "tp"),
        P("fs"),
        P("fs", None),
        P("fs", None),
    )
    return jax.shard_map(
        body,
        mesh=mesh,
        in_specs=placed,
        out_specs=(P("fs", None, "tp"), P("fs", None, "tp"), P("fs", None, "tp"), P("fs", "tp")),
        check_vma=False,
    )
```
